32 devices in a mesh: grp: 2 (over x), ep: 16 (over z, y, core).
Axes of the slice: x: 2, y: 2, z: 4, core: 2. Of those that a mesh axis runs over, the one named last changes fastest.
Arguments:
- tokens: bfloat16 [8192, 2048], P(('grp', 'ep')), parts along dimension 0, may hold values from -6 to 6
- norm_gain: float32 [2048], replicated, may hold values from 0.1 to 1.9
- expert_ids: int32 [8192, 2], P(('grp', 'ep')), parts along dimension 0, may hold values from 0 to 15, all different within a row; in each aligned block of 256 rows (0 to 255, 256 to 511, ...) at most 64 rows name the same one
- gate_weights: float32 [8192, 2], P(('grp', 'ep')), parts along dimension 0, may hold values from 0.1 to 1
- w_gate: bfloat16 [16, 2048, 1024], P('ep'), may hold values from -0.125 to 0.125
- w_up: bfloat16 [16, 2048, 1024], P('ep'), may hold values from -0.125 to 0.125
- w_down: bfloat16 [16, 1024, 2048], P('ep'), may hold values from -0.1875 to 0.1875
Outputs:
- mixed: bfloat16 [8192, 2048], P(('grp', 'ep')), parts along dimension 0
The draws below stay inside these ranges and needn't reach their ends.
There are 2 independent parts, one for each index of `grp`. The reference program is written for one: setup_inputs(seed, part) draws one part's arguments, and reference() takes and returns one part's arrays. A program takes and returns all parts, laid end to end along the dimension named above; an argument that names none is the same for every part. Nothing has to cross between parts.
Inputs may be any that keep to these rules, and one draw needn't show every extreme that they name: `expert_ids`: A token's 2 experts are distinct. Within the rows of one device (aligned blocks of 256 tokens) no expert is named more than 64 times, and in some block one expert is named exactly 64 times.
All inputs are finite; a program needn't handle non-finite values.
Results may differ from the reference program's by a relative error of at most 0.0071.
Values may be sent and summed in bfloat16 or wider, within the bound.
A program may use at most 64 MiB of HBM per device.

```python
import math
import jax
import jax.numpy as jnp
import numpy as np
from jax import lax

D = 2048
FF = 1024
TOP = 2
TOK_DEV = 256
EXPERTS = 16
CAP = 64
TOKENS = 4096
N_EP = 16


def steps_of(stream_key, extent, shards, smallest, high):
    def one(axis_at, shards_of):
        draws = jax.random.uniform(jax.random.fold_in(jax.random.fold_in(stream_key, 6), axis_at), (shards_of,), jnp.float32, smallest / len(shards), high / len(shards))
        return jnp.repeat(jnp.exp(draws), extent[axis_at] // shards_of).reshape((-1,) + (1,) * (len(extent) - axis_at - 1))

    level = one(*shards[0])
    for cut in shards[1:]:
        level = level * one(*cut)
    return level


def shared_out(own_key, own, number, rows, amount, top, bound, lean):
    ranking = jax.random.permutation(own_key, amount)
    heavy_load, common = shares(amount, rows * top, bound, lean, True), shares(amount, rows * top, bound, lean, False)
    places = jnp.arange(amount)

    def named(lengths, rotation):
        used = int((lengths > 0).sum())
        fixed = max(1, used // 4)
        shifted = fixed + (places - fixed + rotation * (used - fixed)) % max(1, amount - fixed)
        return jnp.zeros((amount,), jnp.int32).at[ranking[jnp.where(places < fixed, places, shifted)]].set(jnp.asarray(lengths, jnp.int32))

    lengths = jnp.where(number % 4 == 0, named(heavy_load, number // 4), named(common, number - number // 4 - 1))
    mixed = jax.random.permutation(jax.random.fold_in(own, 3), amount)
    giver, taker = mixed[0:amount // 2 * 2:2], mixed[1:amount // 2 * 2:2]
    margin = jnp.minimum(lengths[giver] - 1, bound - lengths[taker]) // 2
    margin = jnp.where((giver == ranking[0]) | (taker == ranking[0]) | (lengths[taker] == 0), 0, jnp.maximum(margin, 0))
    shifted = jax.random.randint(jax.random.fold_in(own, 4), (amount // 2,), 0, 1 << 20) % (margin + 1)
    lengths = lengths.at[giver].add(-shifted).at[taker].add(shifted)
    members = jnp.searchsorted(jnp.cumsum(lengths), jnp.arange(rows * top), side="right").astype(jnp.int32)
    listing = members.reshape(top, rows).T
    listing = listing[jax.random.permutation(jax.random.fold_in(own, 1), rows)]
    rotation = jax.random.randint(jax.random.fold_in(own, 2), (rows, 1), 0, top)
    return jnp.take_along_axis(listing, (jnp.arange(top)[None, :] + rotation) % top, axis=1)


def shares(count, total, most, skew, full):
    loads = [(1 << 20) // math.isqrt(rank ** skew) + 1 for rank in range(1, count + 1)]
    largest = most if full else min(most, max(-(-total // count), total * loads[0] // sum(loads)))
    least = 1 if total - largest >= count - 1 else 0
    holding, spare = [largest] + [least] * (count - 1), total - largest - least * (count - 1)
    while spare > 0:
        movable = [i for i in range(1, count) if holding[i] < largest] or [i for i in range(1, count) if holding[i] < most]
        mass, remaining = sum([loads[i] for i in movable]), spare
        for i in movable:
            extra = min(most - holding[i], max(1, remaining * loads[i] // mass), spare)
            holding[i] = holding[i] + extra
            spare = spare - extra
    return np.array(holding)


def centred(stream_key, shape, width, reach, split=(), kind=jnp.bfloat16):
    drawn = width * jax.random.normal(stream_key, shape, jnp.float32)
    if split:
        drawn = drawn * steps_of(stream_key, shape, split, -0.22, 0.18)
    return jnp.clip(drawn, -reach, reach).astype(kind)


def setup_inputs(seed: int = 0, part: int = 0) -> dict:
    key_list = jax.random.split(jax.random.key(seed), 8)
    part_splits = jax.random.split(jax.random.fold_in(key_list[7], part), 8)
    tokens = centred(part_splits[0], (TOKENS, D), 1.0, 6.0, ((0, 16),))
    norm_gain = jnp.clip(1.0 + 0.18 * jax.random.normal(key_list[1], (D,), jnp.float32), 0.1, 1.9)
    expert_ids_keys = jax.random.split(jax.random.fold_in(part_splits[2], 1), TOKENS // TOK_DEV)
    expert_ids_turns = jax.random.permutation(jax.random.fold_in(part_splits[2], 3), TOKENS // TOK_DEV)
    expert_ids = jax.vmap(lambda own, number: shared_out(jax.random.fold_in(part_splits[2], 2), own, number, TOK_DEV, EXPERTS, TOP, CAP, 2))(expert_ids_keys, expert_ids_turns).reshape((TOKENS, TOP))
    gate_weights = jnp.clip(0.1 + 0.9 * jax.random.uniform(part_splits[3], (TOKENS, TOP), jnp.float32) ** steps_of(part_splits[3], (TOKENS, TOP), ((0, 16),), -0.2, 0.2), 0.1, 1.0)
    w_gate = centred(key_list[4], (EXPERTS, D, FF), D ** -0.5, 0.125, ((0, 16),))
    w_up = centred(key_list[5], (EXPERTS, D, FF), D ** -0.5, 0.125, ((0, 16),))
    w_down = centred(key_list[6], (EXPERTS, FF, D), FF ** -0.5, 0.1875, ((0, 16),))
    return dict(tokens=tokens, norm_gain=norm_gain, expert_ids=expert_ids, gate_weights=gate_weights, w_gate=w_gate, w_up=w_up, w_down=w_down)


def reference(tokens, norm_gain, expert_ids, gate_weights, w_gate, w_up, w_down):
    values = tokens.astype(jnp.float32)
    normed = (values * lax.rsqrt(lax.optimization_barrier(jnp.mean(values * values, -1, keepdims=True)) + 1e-06) * norm_gain).astype(jnp.bfloat16)
    flat_ids = expert_ids.reshape(N_EP, TOK_DEV * TOP)
    onehot = (flat_ids[:, :, None] == jnp.arange(EXPERTS, dtype=jnp.int32)[None, None, :]).astype(jnp.int32)
    before = jnp.cumsum(onehot, axis=1) - onehot
    slots = lax.optimization_barrier(jnp.sum(onehot * before, axis=-1)).astype(jnp.int32)
    dest = (flat_ids * CAP + slots).astype(jnp.int32)
    copies = jnp.repeat(normed.reshape(N_EP, TOK_DEV, D), TOP, axis=1)
    buffers = jnp.zeros((N_EP, EXPERTS * CAP, D), jnp.bfloat16)
    sources = jnp.arange(N_EP, dtype=jnp.int32)[:, None]
    buffers = buffers.at[sources, dest].set(copies)
    buffers = buffers.reshape(N_EP, EXPERTS, CAP, D).transpose(1, 0, 2, 3).reshape(EXPERTS, N_EP * CAP, D)

    def run(operands):
        rows, gate_w, up_w, down_w = operands
        gate = jnp.dot(rows, gate_w, preferred_element_type=jnp.float32)
        upper = jnp.dot(rows, up_w, preferred_element_type=jnp.float32)
        hidden = (jax.nn.silu(gate) * upper).astype(jnp.bfloat16)
        return jnp.dot(hidden, down_w, preferred_element_type=jnp.float32).astype(jnp.bfloat16)
    results = lax.map(run, (buffers, w_gate, w_up, w_down))
    results = results.reshape(EXPERTS, N_EP, CAP, D).transpose(1, 0, 2, 3).reshape(N_EP, EXPERTS * CAP, D)
    back = jnp.take_along_axis(results, dest[:, :, None], axis=1).astype(jnp.float32)
    back = back.reshape(N_EP, TOK_DEV, TOP, D)
    weights = gate_weights.reshape(N_EP, TOK_DEV, TOP)
    mixed = lax.optimization_barrier(jnp.sum(back * weights[:, :, :, None], axis=2))
    return mixed.reshape(TOKENS, D).astype(jnp.bfloat16)
```

```python
import functools
import jax
import jax.numpy as jnp
from jax import lax
from jax.experimental import pallas as pl
from jax.experimental.pallas import tpu as pltpu
from jax.sharding import PartitionSpec as P

SUB = 4


def kernel(n, cap, tok_ref, gain_ref, ids_ref, gw_ref, wg_ref, wu_ref, wd_ref, out_ref,
           wg, wu, wd, normed, outgoing, arrived, results, returned, hidden, acc,
           send1, recv1, send2, recv2, wsem):
    zs = n // SUB
    me = lax.axis_index("ep")
    hi, lo = me // SUB, me % SUB
    tok, width = tok_ref.shape
    ff = wg.shape[1]
    rows = SUB * cap

    barrier = pltpu.get_barrier_semaphore()

    def greet(r, carry):
        pl.semaphore_signal(barrier, inc=1, device_id={"ep": (me + r) % n},
                            device_id_type=pl.DeviceIdType.MESH)
        return carry

    lax.fori_loop(1, n, greet, 0)
    w_copies = [
        pltpu.make_async_copy(wg_ref.at[0], wg, wsem.at[0]),
        pltpu.make_async_copy(wu_ref.at[0], wu, wsem.at[1]),
        pltpu.make_async_copy(wd_ref.at[0], wd, wsem.at[2]),
    ]
    for c in w_copies:
        c.start()

    ids = ids_ref[...]
    id0, id1 = ids[:, 0:1], ids[:, 1:2]
    lane = lax.broadcasted_iota(jnp.int32, (tok, 128), 1)
    chosen = jnp.where((id0 == lane) | (id1 == lane), 1.0, 0.0)
    t_row = lax.broadcasted_iota(jnp.int32, (tok, tok), 0)
    t_col = lax.broadcasted_iota(jnp.int32, (tok, tok), 1)
    earlier = jnp.where(t_col < t_row, 1.0, 0.0).astype(jnp.bfloat16)
    before = jnp.dot(earlier, chosen.astype(jnp.bfloat16), preferred_element_type=jnp.float32)
    slot0 = jnp.sum(jnp.where(id0 == lane, before, 0.0), axis=1, keepdims=True)
    slot1 = jnp.sum(jnp.where(id1 == lane, before, 0.0), axis=1, keepdims=True)
    dest0 = id0.astype(jnp.float32) * cap + slot0
    dest1 = id1.astype(jnp.float32) * cap + slot1
    both = jnp.where(lane == 0, dest0, jnp.where(lane == 1, dest1, 0.0))
    turned = jnp.transpose(both)
    row0 = turned[0:1, :].astype(jnp.int32)
    row1 = turned[1:2, :].astype(jnp.int32)
    col0 = dest0.astype(jnp.int32)
    col1 = dest1.astype(jnp.int32)

    step = 32

    def norm(i, carry):
        at = pl.ds(pl.multiple_of(i * step, step), step)
        v = tok_ref[at, :].astype(jnp.float32)
        scale = lax.rsqrt(jnp.mean(v * v, -1, keepdims=True) + 1e-06)
        normed[at, :] = (v * scale * gain_ref[...]).astype(jnp.bfloat16)
        return carry

    lax.fori_loop(0, tok // step, norm, 0)

    def shift(j):
        return ((j % 2) * ((j + 1) // 2) + (1 - j % 2) * (zs - j // 2)) % zs

    def target(dz, dl):
        return ((hi + dz) % zs) * SUB + (lo + dl) % SUB

    def source(dz, dl):
        return ((hi - dz + zs) % zs) * SUB + (lo - dl + SUB) % SUB

    def slot_rows(j, dl):
        return pl.ds(pl.multiple_of(j * rows + dl * cap, cap), cap)

    def out_copy(j, dl):
        at = slot_rows(j, dl)
        return pltpu.make_async_remote_copy(
            src_ref=outgoing.at[at, :], dst_ref=arrived.at[at, :],
            send_sem=send1.at[j * SUB + dl], recv_sem=recv1.at[j * SUB + dl],
            device_id={"ep": target(shift(j), dl)}, device_id_type=pl.DeviceIdType.MESH)

    def back_copy(j, dl):
        at = slot_rows(j, dl)
        return pltpu.make_async_remote_copy(
            src_ref=results.at[at, :], dst_ref=returned.at[at, :],
            send_sem=send2.at[j * SUB + dl], recv_sem=recv2.at[j * SUB + dl],
            device_id={"ep": source(shift(j), dl)}, device_id_type=pl.DeviceIdType.MESH)

    def chunk_rows(j):
        return pl.ds(pl.multiple_of(j * rows, rows), rows)

    def pack(j):
        r = lax.broadcasted_iota(jnp.int32, (rows, tok), 0)
        dl, s = r // cap, r % cap
        expert = ((hi + shift(j)) % zs) * SUB + (lo + dl) % SUB
        index = expert * cap + s
        pick = jnp.where((index == row0) | (index == row1), 1.0, 0.0).astype(jnp.bfloat16)
        outgoing[chunk_rows(j), :] = jnp.dot(
            pick, normed[...], preferred_element_type=jnp.float32).astype(jnp.bfloat16)

    def send_out(j):
        for dl in range(SUB):
            out_copy(j, dl).start()

    pack(0)
    pl.semaphore_wait(barrier, n - 1)
    for dl in range(1, SUB):
        out_copy(0, dl).start()
    arrived[0:cap, :] = outgoing[0:cap, :]

    def dispatch(j, carry):
        pack(j)
        send_out(j)
        return carry

    lax.fori_loop(1, zs, dispatch, 0)

    for c in w_copies:
        c.wait()

    ftile = min(ff, 256)
    dtile = min(width, 256)

    def experts(j):
        at = chunk_rows(j)

        def up(f, carry):
            cols = pl.ds(pl.multiple_of(f * ftile, ftile), ftile)
            x = arrived[at, :]
            g = jnp.dot(x, wg[:, cols], preferred_element_type=jnp.float32)
            u = jnp.dot(x, wu[:, cols], preferred_element_type=jnp.float32)
            hidden[:, cols] = (g / (1.0 + jnp.exp(-g)) * u).astype(jnp.bfloat16)
            return carry

        lax.fori_loop(0, ff // ftile, up, 0)

        def down(d, carry):
            cols = pl.ds(pl.multiple_of(d * dtile, dtile), dtile)
            results[at, cols] = jnp.dot(
                hidden[...], wd[:, cols], preferred_element_type=jnp.float32).astype(jnp.bfloat16)
            return carry

        lax.fori_loop(0, width // dtile, down, 0)

    for dl in range(1, SUB):
        out_copy(0, dl).wait_recv()
    experts(0)
    for dl in range(1, SUB):
        back_copy(0, dl).start()
    returned[0:cap, :] = results[0:cap, :]

    def work(j, carry):
        for dl in range(SUB):
            out_copy(j, dl).wait_recv()
        experts(j)
        for dl in range(SUB):
            back_copy(j, dl).start()
        return carry

    lax.fori_loop(1, zs, work, 0)

    gw = gw_ref[...]
    g0, g1 = gw[:, 0:1], gw[:, 1:2]

    def gather(j):
        c = lax.broadcasted_iota(jnp.int32, (tok, rows), 1)
        dl, s = c // cap, c % cap
        expert = ((hi + shift(j)) % zs) * SUB + (lo + dl) % SUB
        index = expert * cap + s
        weight = jnp.where(index == col0, g0, 0.0) + jnp.where(index == col1, g1, 0.0)
        high = weight.astype(jnp.bfloat16)
        low = (weight - high.astype(jnp.float32)).astype(jnp.bfloat16)
        block = returned[chunk_rows(j), :]
        return (jnp.dot(high, block, preferred_element_type=jnp.float32)
                + jnp.dot(low, block, preferred_element_type=jnp.float32))

    for dl in range(1, SUB):
        back_copy(0, dl).wait_recv()
    acc[...] = gather(0)

    def combine(j, carry):
        for dl in range(SUB):
            back_copy(j, dl).wait_recv()
        acc[...] += gather(j)
        return carry

    lax.fori_loop(1, zs - 1, combine, 0)
    for dl in range(SUB):
        back_copy(zs - 1, dl).wait_recv()
    out_ref[...] = (acc[...] + gather(zs - 1)).astype(out_ref.dtype)

    for dl in range(1, SUB):
        out_copy(0, dl).wait_send()
        back_copy(0, dl).wait_send()

    def finish(j, carry):
        for dl in range(SUB):
            out_copy(j, dl).wait_send()
            back_copy(j, dl).wait_send()
        return carry

    lax.fori_loop(1, zs, finish, 0)


def per_device(tokens, norm_gain, expert_ids, gate_weights, w_gate, w_up, w_down):
    n = lax.axis_size("ep")
    tok, width = tokens.shape
    top = expert_ids.shape[1]
    ff = w_gate.shape[2]
    cap = 2 * tok * top // n
    total = n * cap
    bf16 = jnp.bfloat16
    vmem = pl.BlockSpec(memory_space=pltpu.VMEM)
    hbm = pl.BlockSpec(memory_space=pl.ANY)
    return pl.pallas_call(
        functools.partial(kernel, n, cap),
        out_shape=jax.ShapeDtypeStruct((tok, width), bf16),
        in_specs=[vmem] * 4 + [hbm] * 3,
        out_specs=vmem,
        scratch_shapes=[
            pltpu.VMEM((width, ff), bf16),
            pltpu.VMEM((width, ff), bf16),
            pltpu.VMEM((ff, width), bf16),
            pltpu.VMEM((tok, width), bf16),
            pltpu.VMEM((total, width), bf16),
            pltpu.VMEM((total, width), bf16),
            pltpu.VMEM((total, width), bf16),
            pltpu.VMEM((total, width), bf16),
            pltpu.VMEM((SUB * cap, ff), bf16),
            pltpu.VMEM((tok, width), jnp.float32),
            pltpu.SemaphoreType.DMA((n,)),
            pltpu.SemaphoreType.DMA((n,)),
            pltpu.SemaphoreType.DMA((n,)),
            pltpu.SemaphoreType.DMA((n,)),
            pltpu.SemaphoreType.DMA((3,)),
        ],
        compiler_params=pltpu.CompilerParams(
            collective_id=0, has_side_effects=True, vmem_limit_bytes=56 * 1024 * 1024),
    )(tokens, norm_gain.reshape(1, width), expert_ids, gate_weights, w_gate, w_up, w_down)


def solution(mesh):
    return jax.shard_map(
        per_device,
        mesh=mesh,
        in_specs=(
            P(("grp", "ep"), None),
            P(),
            P(("grp", "ep"), None),
            P(("grp", "ep"), None),
            P("ep", None, None),
            P("ep", None, None),
            P("ep", None, None),
        ),
        out_specs=P(("grp", "ep"), None),
        check_vma=False,
    )
```

```python
import functools
import jax
import jax.numpy as jnp
from jax import lax
from jax.experimental import pallas as pl
from jax.experimental.pallas import tpu as pltpu
from jax.sharding import PartitionSpec as P

SUB = 4


def kernel(n, cap, tok_ref, gain_ref, ids_ref, gw_ref, wg_ref, wu_ref, wd_ref, out_ref,
           wg, wu, wd, lines, places, outgoing, arrived, results, returned, hidden, acc,
           send1, recv1, send2, recv2, wsem,
           lsend, lrecv, psend, precv):
    zs = n // SUB
    me = lax.axis_index("ep")
    hi, lo = me // SUB, me % SUB
    tok, width = tok_ref.shape
    ff = wg.shape[1]
    rows = SUB * cap

    barrier = pltpu.get_barrier_semaphore()

    def greet(r, carry):
        pl.semaphore_signal(barrier, inc=1, device_id={"ep": (me + r) % n},
                            device_id_type=pl.DeviceIdType.MESH)
        return carry

    lax.fori_loop(1, n, greet, 0)
    w_copies = [
        pltpu.make_async_copy(wg_ref.at[0], wg, wsem.at[0]),
        pltpu.make_async_copy(wu_ref.at[0], wu, wsem.at[1]),
        pltpu.make_async_copy(wd_ref.at[0], wd, wsem.at[2]),
    ]
    for c in w_copies:
        c.start()

    ids = ids_ref[...]
    id0, id1 = ids[:, 0:1], ids[:, 1:2]
    lane = lax.broadcasted_iota(jnp.int32, (tok, 128), 1)
    chosen = jnp.where((id0 == lane) | (id1 == lane), 1.0, 0.0)
    t_row = lax.broadcasted_iota(jnp.int32, (tok, tok), 0)
    t_col = lax.broadcasted_iota(jnp.int32, (tok, tok), 1)
    earlier = jnp.where(t_col < t_row, 1.0, 0.0).astype(jnp.bfloat16)
    before = jnp.dot(earlier, chosen.astype(jnp.bfloat16), preferred_element_type=jnp.float32)
    slot0 = jnp.sum(jnp.where(id0 == lane, before, 0.0), axis=1, keepdims=True)
    slot1 = jnp.sum(jnp.where(id1 == lane, before, 0.0), axis=1, keepdims=True)
    dest0 = id0.astype(jnp.float32) * cap + slot0
    dest1 = id1.astype(jnp.float32) * cap + slot1
    both = jnp.where(lane == 0, dest0, jnp.where(lane == 1, dest1, 0.0))
    turned = jnp.transpose(both)

    step = 32

    def norm(i, carry):
        at = pl.ds(pl.multiple_of(i * step, step), step)
        v = tok_ref[at, :].astype(jnp.float32)
        scale = lax.rsqrt(jnp.mean(v * v, -1, keepdims=True) + 1e-06)
        lines[hi, at, :] = (v * scale * gain_ref[...]).astype(jnp.bfloat16)
        return carry

    lax.fori_loop(0, tok // step, norm, 0)

    def wait_all(copies):
        for c in copies:
            c.wait_recv()

    def line_copies(block, way):
        to = (hi + 2 * way - 1 + zs) % zs * SUB + lo
        return [
            pltpu.make_async_remote_copy(
                src_ref=buf.at[block], dst_ref=buf.at[block],
                send_sem=sends.at[way * zs + block], recv_sem=recvs.at[block],
                device_id={"ep": to}, device_id_type=pl.DeviceIdType.MESH)
            for buf, sends, recvs in ((places, psend, precv), (lines, lsend, lrecv))
        ]

    def pass_on(block, way):
        for c in line_copies(block, way):
            c.start()

    def slot_rows(j, dl):
        return pl.ds(pl.multiple_of(j * rows + dl * cap, cap), cap)

    def chunk_rows(j):
        return pl.ds(pl.multiple_of(j * rows, rows), rows)

    def out_copy(j, dl):
        at = slot_rows(j, dl)
        return pltpu.make_async_remote_copy(
            src_ref=outgoing.at[at, :], dst_ref=arrived.at[at, :],
            send_sem=send1.at[j * SUB + dl], recv_sem=recv1.at[j * SUB + dl],
            device_id={"ep": hi * SUB + (lo + dl) % SUB}, device_id_type=pl.DeviceIdType.MESH)

    def back_copy(j, dl):
        return pltpu.make_async_remote_copy(
            src_ref=results.at[slot_rows(j, dl), :], dst_ref=returned.at[slot_rows(hi, dl), :],
            send_sem=send2.at[j * SUB + dl], recv_sem=recv2.at[hi * SUB + dl],
            device_id={"ep": j * SUB + (lo - dl + SUB) % SUB}, device_id_type=pl.DeviceIdType.MESH)

    def back_arrival(j, dl):
        at = slot_rows(j, dl)
        return pltpu.make_async_remote_copy(
            src_ref=results.at[at, :], dst_ref=returned.at[at, :],
            send_sem=send2.at[j * SUB + dl], recv_sem=recv2.at[j * SUB + dl],
            device_id={"ep": j * SUB + (lo + dl) % SUB}, device_id_type=pl.DeviceIdType.MESH)

    def pack(j):
        r = lax.broadcasted_iota(jnp.int32, (rows, tok), 0)
        dl, s = r // cap, r % cap
        index = ((hi * SUB + (lo + dl) % SUB) * cap + s).astype(jnp.float32)
        where = places[j]
        pick = jnp.where((index == where[0:1, :]) | (index == where[1:2, :]), 1.0, 0.0)
        outgoing[chunk_rows(j), :] = jnp.dot(
            pick.astype(jnp.bfloat16), lines[j], preferred_element_type=jnp.float32
        ).astype(jnp.bfloat16)
        for dl in range(1, SUB):
            out_copy(j, dl).start()
        arrived[slot_rows(j, 0), :] = outgoing[slot_rows(j, 0), :]

    ftile = min(ff, 256)
    dtile = min(width, 256)

    def experts(j):
        at = chunk_rows(j)
        for dl in range(1, SUB):
            out_copy(j, dl).wait_recv()

        def up(f, carry):
            cols = pl.ds(pl.multiple_of(f * ftile, ftile), ftile)
            x = arrived[at, :]
            g = jnp.dot(x, wg[:, cols], preferred_element_type=jnp.float32)
            u = jnp.dot(x, wu[:, cols], preferred_element_type=jnp.float32)
            hidden[:, cols] = (g / (1.0 + jnp.exp(-g)) * u).astype(jnp.bfloat16)
            return carry

        lax.fori_loop(0, ff // ftile, up, 0)

        def down(d, carry):
            cols = pl.ds(pl.multiple_of(d * dtile, dtile), dtile)
            results[at, cols] = jnp.dot(
                hidden[...], wd[:, cols], preferred_element_type=jnp.float32).astype(jnp.bfloat16)
            return carry

        lax.fori_loop(0, width // dtile, down, 0)
        for dl in range(1, SUB):
            back_copy(j, dl).start()

        @pl.when(j == hi)
        def _():
            returned[slot_rows(hi, 0), :] = results[slot_rows(hi, 0), :]

        @pl.when(j != hi)
        def _():
            back_copy(j, 0).start()

    def both_sides(s, act):
        @pl.when(hi - s >= 0)
        def _():
            act((hi - s + zs) % zs, 1)

        @pl.when(hi + s < zs)
        def _():
            act((hi + s) % zs, 0)

    def forward(block, way):
        @pl.when(hi < zs - 1 if way else hi > 0)
        def _():
            pass_on(block, way)

    def line_arrival(block, way):
        wait_all(line_copies(block, way))

    where = lax.broadcasted_iota(jnp.int32, (8, tok), 0)
    places[hi] = jnp.where(where == 0, turned[0:1, :], turned[1:2, :])
    pl.semaphore_wait(barrier, n - 1)
    forward(hi, 1)
    forward(hi, 0)
    pack(hi)
    for c in w_copies:
        c.wait()

    def step_in(s, carry):
        def take(block, way):
            line_arrival(block, way)
            forward(block, way)

        both_sides(s, take)
        both_sides(s, lambda block, way: pack(block))

        @pl.when(s == 1)
        def _():
            experts(hi)

        @pl.when(s > 1)
        def _():
            both_sides(s - 1, lambda block, way: experts(block))

        return carry

    lax.fori_loop(1, zs, step_in, 0)
    both_sides(zs - 1, lambda block, way: experts(block))

    gw = gw_ref[...]
    g0, g1 = gw[:, 0:1], gw[:, 1:2]

    def gather(j):
        c = lax.broadcasted_iota(jnp.int32, (tok, rows), 1)
        dl, s = c // cap, c % cap
        index = ((j * SUB + (lo + dl) % SUB) * cap + s).astype(jnp.float32)
        weight = jnp.where(index == dest0, g0, 0.0) + jnp.where(index == dest1, g1, 0.0)
        high = weight.astype(jnp.bfloat16)
        low = (weight - high.astype(jnp.float32)).astype(jnp.bfloat16)
        block = returned[chunk_rows(j), :]
        return (jnp.dot(high, block, preferred_element_type=jnp.float32)
                + jnp.dot(low, block, preferred_element_type=jnp.float32))

    wait_all([back_arrival(hi, dl) for dl in range(1, SUB)])
    acc[...] = gather(hi)

    def combine(s, carry):
        def add(block, way):
            wait_all([back_arrival(block, dl) for dl in range(SUB)])
            acc[...] += gather(block)

        both_sides(s, add)
        return carry

    lax.fori_loop(1, zs, combine, 0)
    out_ref[...] = acc[...].astype(out_ref.dtype)

    def finish(j, carry):
        for dl in range(1, SUB):
            out_copy(j, dl).wait_send()
            back_copy(j, dl).wait_send()

        @pl.when(j != hi)
        def _():
            back_copy(j, 0).wait_send()

        for way in (0, 1):
            @pl.when((hi < zs - 1) & (j <= hi) if way else (hi > 0) & (j >= hi))
            def _():
                for c in line_copies(j, way):
                    c.wait_send()

        return carry

    lax.fori_loop(0, zs, finish, 0)


def per_device(tokens, norm_gain, expert_ids, gate_weights, w_gate, w_up, w_down):
    n = lax.axis_size("ep")
    tok, width = tokens.shape
    top = expert_ids.shape[1]
    ff = w_gate.shape[2]
    cap = 2 * tok * top // n
    total = n * cap
    bf16 = jnp.bfloat16
    vmem = pl.BlockSpec(memory_space=pltpu.VMEM)
    hbm = pl.BlockSpec(memory_space=pl.ANY)
    return pl.pallas_call(
        functools.partial(kernel, n, cap),
        out_shape=jax.ShapeDtypeStruct((tok, width), bf16),
        in_specs=[vmem] * 4 + [hbm] * 3,
        out_specs=vmem,
        scratch_shapes=[
            pltpu.VMEM((width, ff), bf16),
            pltpu.VMEM((width, ff), bf16),
            pltpu.VMEM((ff, width), bf16),
            pltpu.VMEM((n // SUB, tok, width), bf16),
            pltpu.VMEM((n // SUB, 8, tok), jnp.float32),
            pltpu.VMEM((total, width), bf16),
            pltpu.VMEM((total, width), bf16),
            pltpu.VMEM((total, width), bf16),
            pltpu.VMEM((total, width), bf16),
            pltpu.VMEM((SUB * cap, ff), bf16),
            pltpu.VMEM((tok, width), jnp.float32),
            pltpu.SemaphoreType.DMA((n,)),
            pltpu.SemaphoreType.DMA((n,)),
            pltpu.SemaphoreType.DMA((n,)),
            pltpu.SemaphoreType.DMA((n,)),
            pltpu.SemaphoreType.DMA((3,)),
            pltpu.SemaphoreType.DMA((2 * n // SUB,)),
            pltpu.SemaphoreType.DMA((n // SUB,)),
            pltpu.SemaphoreType.DMA((2 * n // SUB,)),
            pltpu.SemaphoreType.DMA((n // SUB,)),
        ],
        compiler_params=pltpu.CompilerParams(
            collective_id=0, has_side_effects=True, vmem_limit_bytes=56 * 1024 * 1024),
    )(tokens, norm_gain.reshape(1, width), expert_ids, gate_weights, w_gate, w_up, w_down)


def solution(mesh):
    return jax.shard_map(
        per_device,
        mesh=mesh,
        in_specs=(
            P(("grp", "ep"), None),
            P(),
            P(("grp", "ep"), None),
            P(("grp", "ep"), None),
            P("ep", None, None),
            P("ep", None, None),
            P("ep", None, None),
        ),
        out_specs=P(("grp", "ep"), None),
        check_vma=False,
    )
```

```python
import functools
import jax
import jax.numpy as jnp
from jax import lax
from jax.experimental import pallas as pl
from jax.experimental.pallas import tpu as pltpu
from jax.sharding import PartitionSpec as P

SUB = 4


def kernel(n, cap, tok_ref, gain_ref, ids_ref, gw_ref, wg_ref, wu_ref, wd_ref, out_ref,
           wg, wu, wd, lines, places, outgoing, arrived, results, returned, hidden, acc,
           send1, recv1, send2, recv2, wsem,
           lsend, lrecv, psend, precv):
    zs = n // SUB
    me = lax.axis_index("ep")
    hi, lo = me // SUB, me % SUB
    tok, width = tok_ref.shape
    ff = wg.shape[1]
    rows = SUB * cap

    barrier = pltpu.get_barrier_semaphore()

    def greet(r, carry):
        pl.semaphore_signal(barrier, inc=1, device_id={"ep": (me + r) % n},
                            device_id_type=pl.DeviceIdType.MESH)
        return carry

    lax.fori_loop(1, n, greet, 0)
    w_copies = [
        pltpu.make_async_copy(wg_ref.at[0], wg, wsem.at[0]),
        pltpu.make_async_copy(wu_ref.at[0], wu, wsem.at[1]),
        pltpu.make_async_copy(wd_ref.at[0], wd, wsem.at[2]),
    ]
    for c in w_copies:
        c.start()

    ids = ids_ref[...]
    id0, id1 = ids[:, 0:1], ids[:, 1:2]
    lane = lax.broadcasted_iota(jnp.int32, (tok, 128), 1)
    chosen = jnp.where((id0 == lane) | (id1 == lane), 1.0, 0.0)
    t_row = lax.broadcasted_iota(jnp.int32, (tok, tok), 0)
    t_col = lax.broadcasted_iota(jnp.int32, (tok, tok), 1)
    earlier = jnp.where(t_col < t_row, 1.0, 0.0).astype(jnp.bfloat16)
    before = jnp.dot(earlier, chosen.astype(jnp.bfloat16), preferred_element_type=jnp.float32)
    slot0 = jnp.sum(jnp.where(id0 == lane, before, 0.0), axis=1, keepdims=True)
    slot1 = jnp.sum(jnp.where(id1 == lane, before, 0.0), axis=1, keepdims=True)
    dest0 = id0.astype(jnp.float32) * cap + slot0
    dest1 = id1.astype(jnp.float32) * cap + slot1
    both = jnp.where(lane == 0, dest0, jnp.where(lane == 1, dest1, 0.0))
    turned = jnp.transpose(both)

    step = 32

    def norm(i, carry):
        at = pl.ds(pl.multiple_of(i * step, step), step)
        v = tok_ref[at, :].astype(jnp.float32)
        scale = lax.rsqrt(jnp.mean(v * v, -1, keepdims=True) + 1e-06)
        lines[hi, at, :] = (v * scale * gain_ref[...]).astype(jnp.bfloat16)
        return carry

    lax.fori_loop(0, tok // step, norm, 0)

    def wait_all(copies):
        for c in copies:
            c.wait_recv()

    def line_copies(block, way):
        to = (hi + 2 * way - 1 + zs) % zs * SUB + lo
        return [
            pltpu.make_async_remote_copy(
                src_ref=buf.at[block], dst_ref=buf.at[block],
                send_sem=sends.at[way * zs + block], recv_sem=recvs.at[block],
                device_id={"ep": to}, device_id_type=pl.DeviceIdType.MESH)
            for buf, sends, recvs in ((places, psend, precv), (lines, lsend, lrecv))
        ]

    def pass_on(block, way):
        for c in line_copies(block, way):
            c.start()

    def slot_rows(j, dl):
        return pl.ds(pl.multiple_of(j * rows + dl * cap, cap), cap)

    def chunk_rows(j):
        return pl.ds(pl.multiple_of(j * rows, rows), rows)

    def out_copy(j, dl):
        at = slot_rows(j, dl)
        return pltpu.make_async_remote_copy(
            src_ref=outgoing.at[at, :], dst_ref=arrived.at[at, :],
            send_sem=send1.at[j * SUB + dl], recv_sem=recv1.at[j * SUB + dl],
            device_id={"ep": hi * SUB + (lo + dl) % SUB}, device_id_type=pl.DeviceIdType.MESH)

    def back_copy(j, dl):
        return pltpu.make_async_remote_copy(
            src_ref=results.at[slot_rows(j, dl), :], dst_ref=returned.at[slot_rows(hi, dl), :],
            send_sem=send2.at[j * SUB + dl], recv_sem=recv2.at[hi * SUB + dl],
            device_id={"ep": j * SUB + (lo - dl + SUB) % SUB}, device_id_type=pl.DeviceIdType.MESH)

    def back_arrival(j, dl):
        at = slot_rows(j, dl)
        return pltpu.make_async_remote_copy(
            src_ref=results.at[at, :], dst_ref=returned.at[at, :],
            send_sem=send2.at[j * SUB + dl], recv_sem=recv2.at[j * SUB + dl],
            device_id={"ep": j * SUB + (lo + dl) % SUB}, device_id_type=pl.DeviceIdType.MESH)

    def pack(j):
        r = lax.broadcasted_iota(jnp.int32, (rows, tok), 0)
        dl, s = r // cap, r % cap
        index = ((hi * SUB + (lo + dl) % SUB) * cap + s).astype(jnp.float32)
        where = places[j]
        pick = jnp.where((index == where[0:1, :]) | (index == where[1:2, :]), 1.0, 0.0)
        outgoing[chunk_rows(j), :] = jnp.dot(
            pick.astype(jnp.bfloat16), lines[j], preferred_element_type=jnp.float32
        ).astype(jnp.bfloat16)
        for dl in range(1, SUB):
            out_copy(j, dl).start()
        arrived[slot_rows(j, 0), :] = outgoing[slot_rows(j, 0), :]

    ftile = min(ff, 256)
    dtile = min(width, 256)

    def experts(j):
        at = chunk_rows(j)
        for dl in range(1, SUB):
            out_copy(j, dl).wait_recv()

        def up(f, carry):
            cols = pl.ds(pl.multiple_of(f * ftile, ftile), ftile)
            x = arrived[at, :]
            g = jnp.dot(x, wg[:, cols], preferred_element_type=jnp.float32)
            u = jnp.dot(x, wu[:, cols], preferred_element_type=jnp.float32)
            hidden[:, cols] = (g / (1.0 + jnp.exp(-g)) * u).astype(jnp.bfloat16)
            return carry

        lax.fori_loop(0, ff // ftile, up, 0)

        def down(d, carry):
            cols = pl.ds(pl.multiple_of(d * dtile, dtile), dtile)
            results[at, cols] = jnp.dot(
                hidden[...], wd[:, cols], preferred_element_type=jnp.float32).astype(jnp.bfloat16)
            return carry

        lax.fori_loop(0, width // dtile, down, 0)
        for dl in range(1, SUB):
            back_copy(j, dl).start()

        @pl.when(j == hi)
        def _():
            returned[slot_rows(hi, 0), :] = results[slot_rows(hi, 0), :]

        @pl.when(j != hi)
        def _():
            back_copy(j, 0).start()

    def both_sides(s, act):
        @pl.when(hi - s >= 0)
        def _():
            act((hi - s + zs) % zs, 1)

        @pl.when(hi + s < zs)
        def _():
            act((hi + s) % zs, 0)

    def forward(block, way):
        @pl.when(hi < zs - 1 if way else hi > 0)
        def _():
            pass_on(block, way)

    def line_arrival(block, way):
        wait_all(line_copies(block, way))

    where = lax.broadcasted_iota(jnp.int32, (8, tok), 0)
    places[hi] = jnp.where(where == 0, turned[0:1, :], turned[1:2, :])
    pl.semaphore_wait(barrier, n - 1)
    forward(hi, 1)
    forward(hi, 0)
    pack(hi)
    for c in w_copies:
        c.wait()

    experts(hi)

    side = 1 - 2 * (hi // ((zs + 1) // 2))

    def along(s, act):
        block = hi + side * s

        @pl.when((block >= 0) & (block < zs))
        def _():
            act((block + zs) % zs)

    def step_in(s, carry):
        def take(block, way):
            line_arrival(block, way)
            forward(block, way)

        both_sides(s, take)
        along(s, pack)
        along(-s, pack)

        @pl.when(s > 1)
        def _():
            along(1 - s, experts)

        along(s, experts)
        return carry

    lax.fori_loop(1, zs, step_in, 0)
    along(1 - zs, experts)

    gw = gw_ref[...]
    g0, g1 = gw[:, 0:1], gw[:, 1:2]

    def gather(j):
        c = lax.broadcasted_iota(jnp.int32, (tok, rows), 1)
        dl, s = c // cap, c % cap
        index = ((j * SUB + (lo + dl) % SUB) * cap + s).astype(jnp.float32)
        weight = jnp.where(index == dest0, g0, 0.0) + jnp.where(index == dest1, g1, 0.0)
        high = weight.astype(jnp.bfloat16)
        low = (weight - high.astype(jnp.float32)).astype(jnp.bfloat16)
        block = returned[chunk_rows(j), :]
        return (jnp.dot(high, block, preferred_element_type=jnp.float32)
                + jnp.dot(low, block, preferred_element_type=jnp.float32))

    wait_all([back_arrival(hi, dl) for dl in range(1, SUB)])
    acc[...] = gather(hi)

    def combine(s, carry):
        def add(block, way):
            wait_all([back_arrival(block, dl) for dl in range(SUB)])
            acc[...] += gather(block)

        both_sides(s, add)
        return carry

    lax.fori_loop(1, zs, combine, 0)
    out_ref[...] = acc[...].astype(out_ref.dtype)

    def finish(j, carry):
        for dl in range(1, SUB):
            out_copy(j, dl).wait_send()
            back_copy(j, dl).wait_send()

        @pl.when(j != hi)
        def _():
            back_copy(j, 0).wait_send()

        for way in (0, 1):
            @pl.when((hi < zs - 1) & (j <= hi) if way else (hi > 0) & (j >= hi))
            def _():
                for c in line_copies(j, way):
                    c.wait_send()

        return carry

    lax.fori_loop(0, zs, finish, 0)


def per_device(tokens, norm_gain, expert_ids, gate_weights, w_gate, w_up, w_down):
    n = lax.axis_size("ep")
    tok, width = tokens.shape
    top = expert_ids.shape[1]
    ff = w_gate.shape[2]
    cap = 2 * tok * top // n
    total = n * cap
    bf16 = jnp.bfloat16
    vmem = pl.BlockSpec(memory_space=pltpu.VMEM)
    hbm = pl.BlockSpec(memory_space=pl.ANY)
    return pl.pallas_call(
        functools.partial(kernel, n, cap),
        out_shape=jax.ShapeDtypeStruct((tok, width), bf16),
        in_specs=[vmem] * 4 + [hbm] * 3,
        out_specs=vmem,
        scratch_shapes=[
            pltpu.VMEM((width, ff), bf16),
            pltpu.VMEM((width, ff), bf16),
            pltpu.VMEM((ff, width), bf16),
            pltpu.VMEM((n // SUB, tok, width), bf16),
            pltpu.VMEM((n // SUB, 8, tok), jnp.float32),
            pltpu.VMEM((total, width), bf16),
            pltpu.VMEM((total, width), bf16),
            pltpu.VMEM((total, width), bf16),
            pltpu.VMEM((total, width), bf16),
            pltpu.VMEM((SUB * cap, ff), bf16),
            pltpu.VMEM((tok, width), jnp.float32),
            pltpu.SemaphoreType.DMA((n,)),
            pltpu.SemaphoreType.DMA((n,)),
            pltpu.SemaphoreType.DMA((n,)),
            pltpu.SemaphoreType.DMA((n,)),
            pltpu.SemaphoreType.DMA((3,)),
            pltpu.SemaphoreType.DMA((2 * n // SUB,)),
            pltpu.SemaphoreType.DMA((n // SUB,)),
            pltpu.SemaphoreType.DMA((2 * n // SUB,)),
            pltpu.SemaphoreType.DMA((n // SUB,)),
        ],
        compiler_params=pltpu.CompilerParams(
            collective_id=0, has_side_effects=True, vmem_limit_bytes=56 * 1024 * 1024),
    )(tokens, norm_gain.reshape(1, width), expert_ids, gate_weights, w_gate, w_up, w_down)


def solution(mesh):
    return jax.shard_map(
        per_device,
        mesh=mesh,
        in_specs=(
            P(("grp", "ep"), None),
            P(),
            P(("grp", "ep"), None),
            P(("grp", "ep"), None),
            P("ep", None, None),
            P("ep", None, None),
            P("ep", None, None),
        ),
        out_specs=P(("grp", "ep"), None),
        check_vma=False,
    )
```

```python
import functools
import jax
import jax.numpy as jnp
from jax import lax
from jax.experimental import pallas as pl
from jax.experimental.pallas import tpu as pltpu
from jax.sharding import PartitionSpec as P

SUB = 4
HALVES = 2


def kernel(n, cap, tok_ref, gain_ref, ids_ref, gw_ref, wg_ref, wu_ref, wd_ref, out_ref,
           wg, wu, wd, lines, places, outgoing, arrived, results, returned, hidden, acc,
           send1, recv1, send2, recv2, wsem,
           lsend, lrecv, psend, precv,
           relay, dense, landed, rsend, rrecv, dsend, drecv):
    zs = n // SUB
    me = lax.axis_index("ep")
    hi, lo = me // SUB, me % SUB
    tok, width = tok_ref.shape
    ff = wg.shape[1]
    rows = SUB * cap

    barrier = pltpu.get_barrier_semaphore()

    def greet(r, carry):
        pl.semaphore_signal(barrier, inc=1, device_id={"ep": (me + r) % n},
                            device_id_type=pl.DeviceIdType.MESH)
        return carry

    lax.fori_loop(1, n, greet, 0)
    w_copies = [
        pltpu.make_async_copy(wg_ref.at[0], wg, wsem.at[0]),
        pltpu.make_async_copy(wu_ref.at[0], wu, wsem.at[1]),
        pltpu.make_async_copy(wd_ref.at[0], wd, wsem.at[2]),
    ]
    for c in w_copies:
        c.start()

    ids = ids_ref[...]
    id0, id1 = ids[:, 0:1], ids[:, 1:2]
    lane = lax.broadcasted_iota(jnp.int32, (tok, 128), 1)
    chosen = jnp.where((id0 == lane) | (id1 == lane), 1.0, 0.0)
    t_row = lax.broadcasted_iota(jnp.int32, (tok, tok), 0)
    t_col = lax.broadcasted_iota(jnp.int32, (tok, tok), 1)
    earlier = jnp.where(t_col < t_row, 1.0, 0.0).astype(jnp.bfloat16)
    before = jnp.dot(earlier, chosen.astype(jnp.bfloat16), preferred_element_type=jnp.float32)
    slot0 = jnp.sum(jnp.where(id0 == lane, before, 0.0), axis=1, keepdims=True)
    slot1 = jnp.sum(jnp.where(id1 == lane, before, 0.0), axis=1, keepdims=True)
    dest0 = id0.astype(jnp.float32) * cap + slot0
    dest1 = id1.astype(jnp.float32) * cap + slot1
    gw = gw_ref[...]
    g0, g1 = gw[:, 0:1], gw[:, 1:2]
    both = jnp.where(lane == 0, dest0, jnp.where(
        lane == 1, dest1, jnp.where(lane == 2, g0, jnp.where(lane == 3, g1, 0.0))))
    turned = jnp.transpose(both)

    step = 32

    def norm(i, carry):
        at = pl.ds(pl.multiple_of(i * step, step), step)
        v = tok_ref[at, :].astype(jnp.float32)
        scale = lax.rsqrt(jnp.mean(v * v, -1, keepdims=True) + 1e-06)
        lines[hi, at, :] = (v * scale * gain_ref[...]).astype(jnp.bfloat16)
        return carry

    lax.fori_loop(0, tok // step, norm, 0)

    def wait_all(copies):
        for c in copies:
            c.wait_recv()

    def line_copies(block, way):
        to = (hi + 2 * way - 1 + zs) % zs * SUB + lo
        return [
            pltpu.make_async_remote_copy(
                src_ref=buf.at[block], dst_ref=buf.at[block],
                send_sem=sends.at[way * zs + block], recv_sem=recvs.at[block],
                device_id={"ep": to}, device_id_type=pl.DeviceIdType.MESH)
            for buf, sends, recvs in ((places, psend, precv), (lines, lsend, lrecv))
        ]

    def pass_on(block, way):
        for c in line_copies(block, way):
            c.start()

    def slot_rows(j, dl):
        return pl.ds(pl.multiple_of(j * rows + dl * cap, cap), cap)

    def chunk_rows(j):
        return pl.ds(pl.multiple_of(j * rows, rows), rows)

    def out_copy(j, dl):
        at = slot_rows(j, dl)
        return pltpu.make_async_remote_copy(
            src_ref=outgoing.at[at, :], dst_ref=arrived.at[at, :],
            send_sem=send1.at[j * SUB + dl], recv_sem=recv1.at[j * SUB + dl],
            device_id={"ep": hi * SUB + (lo + dl) % SUB}, device_id_type=pl.DeviceIdType.MESH)

    def back_copy(j, dl):
        return pltpu.make_async_remote_copy(
            src_ref=results.at[slot_rows(j, dl), :], dst_ref=returned.at[slot_rows(hi, dl), :],
            send_sem=send2.at[j * SUB + dl], recv_sem=recv2.at[hi * SUB + dl],
            device_id={"ep": j * SUB + (lo - dl + SUB) % SUB}, device_id_type=pl.DeviceIdType.MESH)

    def back_arrival(j, dl):
        at = slot_rows(j, dl)
        return pltpu.make_async_remote_copy(
            src_ref=results.at[at, :], dst_ref=returned.at[at, :],
            send_sem=send2.at[j * SUB + dl], recv_sem=recv2.at[j * SUB + dl],
            device_id={"ep": j * SUB + (lo + dl) % SUB}, device_id_type=pl.DeviceIdType.MESH)

    def pack(j):
        r = lax.broadcasted_iota(jnp.int32, (rows, tok), 0)
        dl, s = r // cap, r % cap
        index = ((hi * SUB + (lo + dl) % SUB) * cap + s).astype(jnp.float32)
        where = places[j]
        pick = jnp.where((index == where[0:1, :]) | (index == where[1:2, :]), 1.0, 0.0)
        outgoing[chunk_rows(j), :] = jnp.dot(
            pick.astype(jnp.bfloat16), lines[j], preferred_element_type=jnp.float32
        ).astype(jnp.bfloat16)
        for dl in range(1, SUB):
            out_copy(j, dl).start()
        arrived[slot_rows(j, 0), :] = outgoing[slot_rows(j, 0), :]

    upper = hi // (zs - 2)
    meet = upper * (zs - 2) + (1 - upper)
    part = upper * (hi - (zs - 2)) + (1 - upper) * (1 - hi)
    half = width // HALVES

    def direct(plane, block):
        return jnp.logical_not(((plane >= zs - 2) & (block < zs - 2)) | ((plane <= 1) & (block > 1)))

    def relay_copy(j, dl, h):
        at = j - 2 * (1 - upper)
        cols = pl.ds(h * half, half)
        return pltpu.make_async_remote_copy(
            src_ref=results.at[slot_rows(j, dl), cols],
            dst_ref=relay.at[part, slot_rows(at, dl), cols],
            send_sem=rsend.at[(at * SUB + dl) * HALVES + h],
            recv_sem=rrecv.at[((part * (zs - 2) + at) * SUB + dl) * HALVES + h],
            device_id={"ep": meet * SUB + (lo - dl + SUB) % SUB},
            device_id_type=pl.DeviceIdType.MESH)

    def relay_arrival(p, at, dl, h):
        cols = pl.ds(h * half, half)
        sem = ((p * (zs - 2) + at) * SUB + dl) * HALVES + h
        return pltpu.make_async_remote_copy(
            src_ref=relay.at[p, slot_rows(at, dl), cols],
            dst_ref=relay.at[p, slot_rows(at, dl), cols],
            send_sem=rsend.at[(at * SUB + dl) * HALVES + h], recv_sem=rrecv.at[sem],
            device_id={"ep": meet * SUB + (lo + 1) % SUB}, device_id_type=pl.DeviceIdType.MESH)

    def dense_copy(at, h):
        cols = pl.ds(h * half, half)
        return pltpu.make_async_remote_copy(
            src_ref=dense.at[at, :, cols], dst_ref=landed.at[upper, :, cols],
            send_sem=dsend.at[at * HALVES + h], recv_sem=drecv.at[upper * HALVES + h],
            device_id={"ep": (at + 2 * (1 - upper)) * SUB + lo},
            device_id_type=pl.DeviceIdType.MESH)

    def dense_arrival(end, h):
        cols = pl.ds(h * half, half)
        return pltpu.make_async_remote_copy(
            src_ref=landed.at[end, :, cols], dst_ref=landed.at[end, :, cols],
            send_sem=dsend.at[h], recv_sem=drecv.at[end * HALVES + h],
            device_id={"ep": (me + 1) % n}, device_id_type=pl.DeviceIdType.MESH)

    ftile = min(ff, 256)
    dtile = min(width, 256)

    def experts(j):
        at = chunk_rows(j)
        for dl in range(1, SUB):
            out_copy(j, dl).wait_recv()

        def up(f, carry):
            cols = pl.ds(pl.multiple_of(f * ftile, ftile), ftile)
            x = arrived[at, :]
            g = jnp.dot(x, wg[:, cols], preferred_element_type=jnp.float32)
            u = jnp.dot(x, wu[:, cols], preferred_element_type=jnp.float32)
            hidden[:, cols] = (g / (1.0 + jnp.exp(-g)) * u).astype(jnp.bfloat16)
            return carry

        lax.fori_loop(0, ff // ftile, up, 0)

        def down(d, carry):
            cols = pl.ds(pl.multiple_of(d * dtile, dtile), dtile)
            results[at, cols] = jnp.dot(
                hidden[...], wd[:, cols], preferred_element_type=jnp.float32).astype(jnp.bfloat16)
            return carry

        lax.fori_loop(0, width // dtile, down, 0)

        @pl.when(direct(hi, j))
        def _():
            for dl in range(1, SUB):
                back_copy(j, dl).start()

        @pl.when(j == hi)
        def _():
            returned[slot_rows(hi, 0), :] = results[slot_rows(hi, 0), :]

        @pl.when((j != hi) & direct(hi, j))
        def _():
            back_copy(j, 0).start()

        @pl.when(jnp.logical_not(direct(hi, j)))
        def _():
            for h in range(HALVES):
                for dl in range(1, SUB):
                    relay_copy(j, dl, h).start()

                @pl.when(hi != meet)
                def _():
                    relay_copy(j, 0, h).start()

            @pl.when(hi == meet)
            def _():
                relay[0, slot_rows(j - 2 * (1 - upper), 0), :] = results[slot_rows(j, 0), :]

    def both_sides(s, act):
        @pl.when(hi - s >= 0)
        def _():
            act((hi - s + zs) % zs, 1)

        @pl.when(hi + s < zs)
        def _():
            act((hi + s) % zs, 0)

    def forward(block, way):
        @pl.when(hi < zs - 1 if way else hi > 0)
        def _():
            pass_on(block, way)

    def line_arrival(block, way):
        wait_all(line_copies(block, way))

    where = lax.broadcasted_iota(jnp.int32, (8, tok), 0)
    places[hi] = jnp.where(
        where == 0, turned[0:1, :], jnp.where(
            where == 1, turned[1:2, :], jnp.where(where == 2, turned[2:3, :], turned[3:4, :])))
    pl.semaphore_wait(barrier, n - 1)
    forward(hi, 1)
    forward(hi, 0)
    pack(hi)
    for c in w_copies:
        c.wait()

    experts(hi)

    side = 1 - 2 * (hi // ((zs + 1) // 2))

    def along(s, act):
        block = hi + side * s

        @pl.when((block >= 0) & (block < zs))
        def _():
            act((block + zs) % zs)

    def step_in(s, carry):
        def take(block, way):
            line_arrival(block, way)
            forward(block, way)

        both_sides(s, take)
        along(s, pack)
        along(-s, pack)

        @pl.when(s > 1)
        def _():
            along(1 - s, experts)

        along(s, experts)
        return carry

    lax.fori_loop(1, zs, step_in, 0)
    along(1 - zs, experts)

    def share(p, at, cols):
        block_places = places[at + 2 * (1 - upper)]
        r = lax.broadcasted_iota(jnp.int32, (rows, tok), 0)
        dl, s = r // cap, r % cap
        plane = upper * (zs - 2 + p) + (1 - upper) * (1 - p)
        index = ((plane * SUB + (lo + dl) % SUB) * cap + s).astype(jnp.float32)
        weight = (jnp.where(index == block_places[0:1, :], block_places[2:3, :], 0.0)
                  + jnp.where(index == block_places[1:2, :], block_places[3:4, :], 0.0))
        high = weight.astype(jnp.bfloat16)
        low = (weight - high.astype(jnp.float32)).astype(jnp.bfloat16)
        block = relay[p, chunk_rows(at), cols]
        dims = (((0,), (0,)), ((), ()))
        return (lax.dot_general(high, block, dims, preferred_element_type=jnp.float32)
                + lax.dot_general(low, block, dims, preferred_element_type=jnp.float32))

    @pl.when(hi == meet)
    def _():
        def meeting(t, carry):
            at = upper * (zs - 3 - t) + (1 - upper) * t
            for h in range(HALVES):
                cols = pl.ds(h * half, half)
                wait_all([relay_arrival(0, at, dl, h) for dl in range(1, SUB)])
                wait_all([relay_arrival(1, at, dl, h) for dl in range(SUB)])
                dense[at, :, cols] = (share(0, at, cols) + share(1, at, cols)).astype(jnp.bfloat16)
                dense_copy(at, h).start()
            return carry

        lax.fori_loop(0, zs - 2, meeting, 0)

    def gather(j):
        c = lax.broadcasted_iota(jnp.int32, (tok, rows), 1)
        dl, s = c // cap, c % cap
        index = ((j * SUB + (lo + dl) % SUB) * cap + s).astype(jnp.float32)
        weight = jnp.where(index == dest0, g0, 0.0) + jnp.where(index == dest1, g1, 0.0)
        high = weight.astype(jnp.bfloat16)
        low = (weight - high.astype(jnp.float32)).astype(jnp.bfloat16)
        block = returned[chunk_rows(j), :]
        return (jnp.dot(high, block, preferred_element_type=jnp.float32)
                + jnp.dot(low, block, preferred_element_type=jnp.float32))

    wait_all([back_arrival(hi, dl) for dl in range(1, SUB)])
    acc[...] = gather(hi)

    def combine(s, carry):
        def add(block, way):
            @pl.when(direct(block, hi))
            def _():
                wait_all([back_arrival(block, dl) for dl in range(SUB)])
                acc[...] += gather(block)

        both_sides(s, add)
        return carry

    lax.fori_loop(1, zs, combine, 0)
    for end in (0, 1):
        @pl.when(hi < zs - 2 if end else hi > 1)
        def _():
            for h in range(HALVES):
                cols = pl.ds(h * half, half)
                dense_arrival(end, h).wait_recv()
                acc[:, cols] += landed[end, :, cols].astype(jnp.float32)
    out_ref[...] = acc[...].astype(out_ref.dtype)

    def finish(j, carry):
        for dl in range(1, SUB):
            out_copy(j, dl).wait_send()

        @pl.when(direct(hi, j))
        def _():
            for dl in range(1, SUB):
                back_copy(j, dl).wait_send()

        @pl.when((j != hi) & direct(hi, j))
        def _():
            back_copy(j, 0).wait_send()

        @pl.when(jnp.logical_not(direct(hi, j)))
        def _():
            for h in range(HALVES):
                for dl in range(1, SUB):
                    relay_copy(j, dl, h).wait_send()

                @pl.when(hi != meet)
                def _():
                    relay_copy(j, 0, h).wait_send()

                @pl.when(hi == meet)
                def _():
                    dense_copy(j - 2 * (1 - upper), h).wait_send()

        for way in (0, 1):
            @pl.when((hi < zs - 1) & (j <= hi) if way else (hi > 0) & (j >= hi))
            def _():
                for c in line_copies(j, way):
                    c.wait_send()

        return carry

    lax.fori_loop(0, zs, finish, 0)


def per_device(tokens, norm_gain, expert_ids, gate_weights, w_gate, w_up, w_down):
    n = lax.axis_size("ep")
    tok, width = tokens.shape
    top = expert_ids.shape[1]
    ff = w_gate.shape[2]
    cap = 2 * tok * top // n
    total = n * cap
    bf16 = jnp.bfloat16
    vmem = pl.BlockSpec(memory_space=pltpu.VMEM)
    hbm = pl.BlockSpec(memory_space=pl.ANY)
    return pl.pallas_call(
        functools.partial(kernel, n, cap),
        out_shape=jax.ShapeDtypeStruct((tok, width), bf16),
        in_specs=[vmem] * 4 + [hbm] * 3,
        out_specs=vmem,
        scratch_shapes=[
            pltpu.VMEM((width, ff), bf16),
            pltpu.VMEM((width, ff), bf16),
            pltpu.VMEM((ff, width), bf16),
            pltpu.VMEM((n // SUB, tok, width), bf16),
            pltpu.VMEM((n // SUB, 8, tok), jnp.float32),
            pltpu.VMEM((total, width), bf16),
            pltpu.VMEM((total, width), bf16),
            pltpu.VMEM((total, width), bf16),
            pltpu.VMEM((total, width), bf16),
            pltpu.VMEM((SUB * cap, ff), bf16),
            pltpu.VMEM((tok, width), jnp.float32),
            pltpu.SemaphoreType.DMA((n,)),
            pltpu.SemaphoreType.DMA((n,)),
            pltpu.SemaphoreType.DMA((n,)),
            pltpu.SemaphoreType.DMA((n,)),
            pltpu.SemaphoreType.DMA((3,)),
            pltpu.SemaphoreType.DMA((2 * n // SUB,)),
            pltpu.SemaphoreType.DMA((n // SUB,)),
            pltpu.SemaphoreType.DMA((2 * n // SUB,)),
            pltpu.SemaphoreType.DMA((n // SUB,)),
            pltpu.VMEM((2, (n // SUB - 2) * SUB * cap, width), bf16),
            pltpu.VMEM((n // SUB - 2, tok, width), bf16),
            pltpu.VMEM((2, tok, width), bf16),
            pltpu.SemaphoreType.DMA(((n - 2 * SUB) * HALVES,)),
            pltpu.SemaphoreType.DMA((2 * (n - 2 * SUB) * HALVES,)),
            pltpu.SemaphoreType.DMA(((n // SUB - 2) * HALVES,)),
            pltpu.SemaphoreType.DMA((2 * HALVES,)),
        ],
        compiler_params=pltpu.CompilerParams(
            collective_id=0, has_side_effects=True, vmem_limit_bytes=62 * 1024 * 1024),
    )(tokens, norm_gain.reshape(1, width), expert_ids, gate_weights, w_gate, w_up, w_down)


def solution(mesh):
    return jax.shard_map(
        per_device,
        mesh=mesh,
        in_specs=(
            P(("grp", "ep"), None),
            P(),
            P(("grp", "ep"), None),
            P(("grp", "ep"), None),
            P("ep", None, None),
            P("ep", None, None),
            P("ep", None, None),
        ),
        out_specs=P(("grp", "ep"), None),
        check_vma=False,
    )
```
